32 devices in a mesh: sp: 8 (over z, y), tp: 4 (over x, core).
Axes of the slice: x: 2, y: 2, z: 4, core: 2. Of those that a mesh axis runs over, the one named last changes fastest.
Arguments:
- queries: bfloat16 [6144, 1536], P('sp', 'tp'), may hold values from -130 to 130, as said below
- keys: bfloat16 [6144, 512], P('sp', 'tp'), may hold values from -6 to 6
- values: bfloat16 [6144, 512], P('sp', 'tp'), may hold values from -6 to 6
- residual: bfloat16 [6144, 2048], P(('sp', 'tp')), may hold values from -6 to 6
- sinks: float32 [12], P('tp'), may hold values from 2 to 6
- out_weight: bfloat16 [1536, 2048], P('tp'), may hold values from -0.15625 to 0.15625
- up_weight: bfloat16 [2048, 8192], P('sp', 'tp'), may hold values from -0.125 to 0.125
- down_weight: bfloat16 [8192, 2048], P('tp', 'sp'), may hold values from -0.0625 to 0.0625
- gains: float32 [2, 2048], replicated, may hold values from 0.1 to 1.9
- biases: float32 [2, 2048], replicated, may hold values from -3 to 3
Outputs:
- layer_out: bfloat16 [6144, 2048], P(('sp', 'tp'))
The draws below stay inside these ranges and needn't reach their ends.
Inputs may be any that keep to these rules, and one draw needn't show every extreme that they name: `queries`: entries of order one, with some rows far larger in some draws.
All inputs are finite; a program needn't handle non-finite values.
Results may differ from the reference program's by a relative error of at most 0.0095.
Values may be sent and summed in bfloat16 or wider, within the bound.
A program may use at most 128 MiB of HBM per device.

```python
import jax
import jax.numpy as jnp
from jax import lax

D = 2048
HEADS = 12
KV_HEADS = 4
HEAD = 128
FF = 8192
WINDOW = 128
TOKENS = 6144
Q_W = 1536
KV_W = 512
N_TP = 4


def base_keys(key):
    drawn = jax.random.normal(jax.random.fold_in(key, 11), (TOKENS, KV_HEADS * HEAD), jnp.float32)
    return jnp.clip(drawn, -6.0, 6.0)


def draw_keys(key, part):
    return base_keys(key).astype(jnp.bfloat16)


def draw_queries(key, part):
    drawn = jnp.clip(jax.random.normal(jax.random.fold_in(key, 12), (TOKENS, HEADS * HEAD), jnp.float32), -6.0, 6.0)
    return drawn.astype(jnp.bfloat16)


def shard_levels(own_key, extent, pieces, low, high):
    level = 1.0
    for axis_at, blocks in pieces:
        steps = jax.random.uniform(jax.random.fold_in(jax.random.fold_in(own_key, 6), axis_at), (blocks,), jnp.float32, low / len(pieces), high / len(pieces))
        level = level * jnp.repeat(jnp.exp(steps), extent[axis_at] // blocks).reshape((-1,) + (1,) * (len(extent) - 1 - axis_at))
    return level


def gaussian(stream_key, shape, scale, limit, split=(), kind=jnp.bfloat16):
    entries = jax.random.normal(stream_key, shape, jnp.float32) * scale
    if len(split) > 0:
        entries = shard_levels(stream_key, shape, split, -0.22, 0.18) * entries
    return jnp.clip(entries, min=-limit, max=limit).astype(kind)


def setup_inputs(seed: int = 0) -> dict:
    streams_of = jax.random.split(jax.random.key(seed), 11)
    return {
        "queries": draw_queries(jax.random.fold_in(streams_of[10], 71), 0),
        "keys": draw_keys(jax.random.fold_in(streams_of[10], 71), 0),
        "values": gaussian(streams_of[2], (TOKENS, KV_W), 1.0, 6.0, ((0, 8), (1, 4))),
        "residual": gaussian(streams_of[3], (TOKENS, D), 1.0, 6.0, ((0, 32),)),
        "sinks": jnp.clip(2.0 + 4.0 * jax.random.uniform(streams_of[4], (HEADS,), jnp.float32) ** shard_levels(streams_of[4], (HEADS,), ((0, 4),), -0.2, 0.2), 2.0, 6.0),
        "out_weight": gaussian(streams_of[5], (Q_W, D), Q_W ** -0.5, 0.15625, ((0, 4),)),
        "up_weight": gaussian(streams_of[6], (D, FF), D ** -0.5, 0.125, ((0, 8), (1, 4))),
        "down_weight": gaussian(streams_of[7], (FF, D), FF ** -0.5, 0.0625, ((0, 4), (1, 8))),
        "gains": jnp.clip(1.0 + 0.18 * jax.random.normal(streams_of[8], (2, D), jnp.float32), 0.1, 1.9),
        "biases": gaussian(streams_of[9], (2, D), 0.5, 3.0, (), jnp.float32),
    }


deep_alpha = 1.6817928
norm_eps = 1e-05
neg_big = -1e+30

def layer_norm(stream, gain, bias):
    mean = lax.optimization_barrier(jnp.mean(stream, axis=-1, keepdims=True))
    spread = lax.optimization_barrier(jnp.mean(jnp.square(stream - mean), axis=-1, keepdims=True))
    return ((stream - mean) * lax.rsqrt(spread + norm_eps) * gain + bias).astype(jnp.bfloat16)

def window_attention(queries, keys, values, sinks):
    total = keys.shape[0]
    blocks = total // WINDOW
    group = HEADS // KV_HEADS
    q_blocks = queries.reshape(blocks, WINDOW, KV_HEADS, group, HEAD).astype(jnp.float32)
    padding = jnp.zeros((WINDOW, KV_HEADS, HEAD), jnp.bfloat16)
    key_ext = jnp.concatenate([padding, keys.reshape(total, KV_HEADS, HEAD)], axis=0)
    val_ext = jnp.concatenate([padding, values.reshape(total, KV_HEADS, HEAD)], axis=0)
    key_win = jnp.concatenate([key_ext[:total].reshape(blocks, WINDOW, KV_HEADS, HEAD), key_ext[WINDOW:].reshape(blocks, WINDOW, KV_HEADS, HEAD)], axis=1)
    val_win = jnp.concatenate([val_ext[:total].reshape(blocks, WINDOW, KV_HEADS, HEAD), val_ext[WINDOW:].reshape(blocks, WINDOW, KV_HEADS, HEAD)], axis=1)
    logits = jnp.einsum('nqkgd,nskd->nkgqs', q_blocks, key_win.astype(jnp.float32)) * HEAD ** (-0.5)
    q_index = jnp.arange(WINDOW, dtype=jnp.int32)[:, None]
    k_index = jnp.arange(2 * WINDOW, dtype=jnp.int32)[None, :]
    dist = q_index + WINDOW - k_index
    block_id = jnp.arange(blocks, dtype=jnp.int32)[:, None, None]
    key_pos = block_id * WINDOW - WINDOW + k_index
    valid = (dist >= 0) & (dist < WINDOW) & (key_pos >= 0)
    heads = jnp.arange(HEADS, dtype=jnp.float32)
    slopes = jnp.exp2(-8.0 * (heads + 1.0) / HEADS).reshape(KV_HEADS, group)[:, :, None, None]
    logits = logits - slopes * dist.astype(jnp.float32)
    logits = jnp.where(valid[:, None, None], logits, neg_big)
    sink = sinks.reshape(KV_HEADS, group)[:, :, None, None]
    top = jnp.maximum(lax.optimization_barrier(jnp.max(logits, axis=-1, keepdims=True)), sink)
    probs = jnp.exp(logits - top)
    denom = lax.optimization_barrier(jnp.sum(probs, axis=-1, keepdims=True)) + jnp.exp(sink - top)
    weight = (probs / denom).astype(jnp.bfloat16)
    attended = jnp.einsum('nkgqs,nskd->nqkgd', weight.astype(jnp.float32), val_win.astype(jnp.float32))
    return attended.astype(jnp.bfloat16).reshape(total, Q_W)

def reference(queries, keys, values, residual, sinks, out_weight, up_weight, down_weight, gains, biases):
    attended = window_attention(queries, keys, values, sinks)
    width = Q_W // N_TP
    mix = jnp.zeros((TOKENS, D), jnp.float32)
    for group_id in range(N_TP):
        term = jnp.dot(attended[:, group_id * width:(group_id + 1) * width], out_weight[group_id * width:(group_id + 1) * width], preferred_element_type=jnp.float32).astype(jnp.bfloat16)
        mix = mix + term.astype(jnp.float32)
    normed = layer_norm(deep_alpha * residual.astype(jnp.float32) + mix, gains[0], biases[0])
    hidden = FF // N_TP
    ffn = jnp.zeros((TOKENS, D), jnp.float32)
    for group_id in range(N_TP):
        upward = jnp.dot(normed, up_weight[:, group_id * hidden:(group_id + 1) * hidden], preferred_element_type=jnp.float32)
        act = jnp.square(jax.nn.relu(upward)).astype(jnp.bfloat16)
        term = jnp.dot(act, down_weight[group_id * hidden:(group_id + 1) * hidden], preferred_element_type=jnp.float32).astype(jnp.bfloat16)
        ffn = ffn + term.astype(jnp.float32)
    return layer_norm(deep_alpha * normed.astype(jnp.float32) + ffn, gains[1], biases[1])
```

```python
import functools

import jax
import jax.numpy as jnp
from jax import lax
from jax.experimental import pallas as pl
from jax.experimental.pallas import tpu as pltpu
from jax.sharding import PartitionSpec as P

HEADS = 12
HEAD = 128
WINDOW = 128


deep_alpha = 1.6817928
norm_eps = 1e-05
neg_big = -1e30


def from_behind(block, axis, distance):
    devices = range(lax.axis_size(axis))
    route = [(i - distance, i) for i in devices if i - distance in devices]
    return lax.ppermute(block, axis, route)


def layer_norm(stream, gain, bias):
    mean = jnp.mean(stream, axis=-1, keepdims=True)
    spread = jnp.mean(jnp.square(stream - mean), axis=-1, keepdims=True)
    return ((stream - mean) * lax.rsqrt(spread + norm_eps) * gain + bias).astype(jnp.bfloat16)


def attend(queries, keys, values, before, sinks, offset, rank_tp):
    tokens = keys.shape[0]
    kv_local = keys.shape[1] // HEAD
    heads_local = sinks.shape[0]
    group = heads_local // kv_local
    blocks = tokens // WINDOW
    q_blocks = queries.reshape(blocks, WINDOW, kv_local, group, HEAD)
    key_ext = jnp.concatenate([before[0], keys], axis=0).reshape(tokens + WINDOW, kv_local, HEAD)
    val_ext = jnp.concatenate([before[1], values], axis=0).reshape(tokens + WINDOW, kv_local, HEAD)
    key_win = jnp.concatenate(
        [
            key_ext[:tokens].reshape(blocks, WINDOW, kv_local, HEAD),
            key_ext[WINDOW:].reshape(blocks, WINDOW, kv_local, HEAD),
        ],
        axis=1,
    )
    val_win = jnp.concatenate(
        [
            val_ext[:tokens].reshape(blocks, WINDOW, kv_local, HEAD),
            val_ext[WINDOW:].reshape(blocks, WINDOW, kv_local, HEAD),
        ],
        axis=1,
    )
    logits = jnp.einsum(
        "nqkgd,nskd->nkgqs", q_blocks, key_win, preferred_element_type=jnp.float32
    ) * HEAD ** (-0.5)
    q_index = jnp.arange(WINDOW, dtype=jnp.int32)[:, None]
    k_index = jnp.arange(2 * WINDOW, dtype=jnp.int32)[None, :]
    dist = q_index + WINDOW - k_index
    block_id = jnp.arange(blocks, dtype=jnp.int32)[:, None, None]
    key_pos = offset + block_id * WINDOW - WINDOW + k_index
    valid = (dist >= 0) & (dist < WINDOW) & (key_pos >= 0)
    heads = (jnp.arange(heads_local, dtype=jnp.int32) + rank_tp * heads_local).astype(jnp.float32)
    slopes = jnp.exp2(-8.0 * (heads + 1.0) / HEADS).reshape(kv_local, group)[:, :, None, None]
    logits = logits - slopes * dist.astype(jnp.float32)
    logits = jnp.where(valid[:, None, None], logits, neg_big)
    sink = sinks.reshape(kv_local, group)[:, :, None, None]
    top = jnp.maximum(jnp.max(logits, axis=-1, keepdims=True), sink)
    probs = jnp.exp(logits - top)
    denom = jnp.sum(probs, axis=-1, keepdims=True) + jnp.exp(sink - top)
    weight = (probs / denom).astype(jnp.bfloat16)
    attended = jnp.einsum("nkgqs,nskd->nqkgd", weight, val_win, preferred_element_type=jnp.float32)
    return attended.astype(jnp.bfloat16).reshape(tokens, heads_local * HEAD)


MESH = pl.DeviceIdType.MESH
LANES = 128


def norm_rows(stream, gain, bias):
    mean = jnp.mean(stream, axis=-1, keepdims=True)
    spread = jnp.mean(jnp.square(stream - mean), axis=-1, keepdims=True)
    return (stream - mean) * lax.rsqrt(spread + norm_eps) * gain + bias


def block_kernel(
    n, m, up_ref, down_ref, mix_ref, res_ref, gains_ref, biases_ref, out_ref,
    up_all, down_all, mix_in, normed, act, terms, terms_in, total,
    ring_send, ring_recv, mix_send, mix_recv, row_send, row_recv, sum_send, sum_recv,
):
    me, rank = lax.axis_index("sp"), lax.axis_index("tp")
    depth, hidden = up_ref.shape
    half = depth // 2
    own_rows, width = res_ref.shape
    step_rows = 32

    odd = lax.rem(me, 2)
    place = (1 - odd) * lax.div(me, 2) + odd * (n - 1 - lax.div(me, 2))

    def member(at):
        at = lax.rem(at + n, n)
        back = lax.div(at, n // 2)
        return (1 - back) * (2 * at) + back * (2 * (n - 1 - at) + 1)

    right, left = member(place + 1), member(place - 1)

    def peer(k):
        return lax.rem(rank + k, m)

    barrier = pltpu.get_barrier_semaphore()
    for there in (left, right):
        pl.semaphore_signal(barrier, inc=1, device_id=(there, rank), device_id_type=MESH)
    for k in range(1, m):
        pl.semaphore_signal(barrier, inc=1, device_id=(me, peer(k)), device_id_type=MESH)
    pl.semaphore_wait(barrier, m + 1)

    def remote(source, target, send, recv, device):
        return pltpu.make_async_remote_copy(
            src_ref=source, dst_ref=target, send_sem=send, recv_sem=recv,
            device_id=device, device_id_type=MESH,
        )

    def hop(which, s, d, c):
        owner = member(place - s) if d == 0 else member(place + s)
        if which == 0:
            rows = half // 2
            off = d * half + c * rows
            target = up_all.at[pl.ds(pl.multiple_of(owner * depth + off, rows), rows)]
            source = up_ref.at[pl.ds(off, rows)] if s == 0 else target
        else:
            rows = hidden // 2
            target = down_all.at[2 * owner + d, pl.ds(c * rows, rows)]
            source = target
            if s == 0:
                source = down_ref.at[pl.ds(c * rows, rows), pl.ds(d * half, half)]
        return remote(
            source, target, ring_send.at[which, s, d, c], ring_recv.at[which, s, d, c],
            (right if d == 0 else left, rank),
        )

    def launch(which):
        for c in range(2):
            for d in range(2):
                hop(which, 0, d, c).start()

    def serve(which, s, c):
        for d in range(2):
            hop(which, s, d, c).wait_recv()
            if s + 1 < n - 1:
                hop(which, s + 1, d, c).start()

    def serve_up(s):
        for c in range(2):
            serve(0, s, c)
        if s == max(n - 3, 0):
            launch(1)

    launch(0)
    mix_copies = [
        remote(
            mix_ref.at[pl.ds(pl.multiple_of(peer(k) * own_rows, own_rows), own_rows)],
            mix_in.at[k - 1], mix_send.at[k - 1], mix_recv.at[k - 1], (me, peer(k)),
        )
        for k in range(1, m)
    ]
    for copy in mix_copies:
        copy.start()
    up_all[pl.ds(pl.multiple_of(me * depth, depth), depth)] = up_ref[...]
    for d in range(2):
        down_all[2 * me + d] = down_ref[:, d * half : (d + 1) * half]

    early = (n - 1) // 2
    for s in range(early):
        serve_up(s)
    for copy in mix_copies:
        copy.wait_recv()

    @pl.loop(0, own_rows // step_rows)
    def _(i):
        start = pl.multiple_of(i * step_rows, step_rows)
        rows = pl.ds(start, step_rows)
        mine = pl.ds(pl.multiple_of(rank * own_rows + start, step_rows), step_rows)
        mix = mix_ref[mine].astype(jnp.float32)
        for k in range(m - 1):
            mix += mix_in[k, rows].astype(jnp.float32)
        stream = deep_alpha * res_ref[rows].astype(jnp.float32) + mix
        normed[mine] = norm_rows(stream, gains_ref[0:1], biases_ref[0:1]).astype(jnp.bfloat16)

    held = pl.ds(pl.multiple_of(rank * own_rows, own_rows), own_rows)
    row_copies = [
        remote(
            normed.at[held], normed.at[held], row_send.at[k - 1], row_recv.at[k - 1], (me, peer(k))
        )
        for k in range(1, m)
    ]
    for copy in row_copies:
        copy.start()
    for s in range(early, n - 1):
        serve_up(s)
    for copy in row_copies:
        copy.wait_recv()

    tile = 256
    tiles = hidden // tile
    parts = 4

    def upward(first, last):
        @pl.loop(first, last)
        def _(i):
            columns = pl.ds(pl.multiple_of(i * tile, tile), tile)
            made = jnp.dot(normed[...], up_all[:, columns], preferred_element_type=jnp.float32)
            act[:, columns] = jnp.square(jnp.maximum(made, 0.0)).astype(jnp.bfloat16)

    for part in range(parts):
        upward(part * tiles // parts, (part + 1) * tiles // parts)
        if part < 2:
            serve(1, 0, part)

    def owners(j):
        return member(place - j), member(place + j)

    def share(j, k):
        return remote(
            terms.at[j, :, pl.ds(pl.multiple_of(peer(k) * own_rows, own_rows), own_rows)],
            terms_in.at[k - 1, j], sum_send.at[k - 1, j], sum_recv.at[k - 1, j], (me, peer(k)),
        )

    def downward(j):
        for d, owner in enumerate(owners(j)):
            terms[j, d] = jnp.dot(
                act[...], down_all[2 * owner + d], preferred_element_type=jnp.float32
            ).astype(jnp.bfloat16)
        for k in range(1, m):
            share(j, k).start()

    def collect(j):
        for k in range(1, m):
            share(j, k).wait_recv()
        for d, owner in enumerate(owners(j)):
            columns = pl.ds(pl.multiple_of(owner * depth + d * half, half), half)
            block = terms[j, d, held].astype(jnp.float32)
            for k in range(m - 1):
                block += terms_in[k, j, d].astype(jnp.float32)
            total[:, columns] = deep_alpha * normed[held, columns].astype(jnp.float32) + block

    downward(0)
    downward(1)
    for s in range(1, n - 1):
        for c in range(2):
            serve(1, s, c)
        downward(s + 1)
        collect(s - 1)
    collect(n - 2)
    collect(n - 1)

    @pl.loop(0, own_rows // step_rows)
    def _(i):
        rows = pl.ds(pl.multiple_of(i * step_rows, step_rows), step_rows)
        out_ref[rows] = norm_rows(total[rows], gains_ref[1:2], biases_ref[1:2]).astype(jnp.bfloat16)

    for copy in mix_copies + row_copies:
        copy.wait_send()
    for j in range(n):
        for k in range(1, m):
            share(j, k).wait_send()
    for which in range(2):
        for s in range(n - 1):
            for d in range(2):
                for c in range(2):
                    hop(which, s, d, c).wait_send()


def fused_block(up_weight, down_weight, mix, residual, gains, biases):
    n, m = lax.axis_size("sp"), lax.axis_size("tp")
    depth, hidden = up_weight.shape
    half = depth // 2
    tokens, width = mix.shape
    own_rows = residual.shape[0]
    bf16, dma = jnp.bfloat16, pltpu.SemaphoreType.DMA
    return pl.pallas_call(
        functools.partial(block_kernel, n, m),
        out_shape=jax.ShapeDtypeStruct(residual.shape, bf16),
        in_specs=[pl.BlockSpec(memory_space=pltpu.VMEM)] * 6,
        out_specs=pl.BlockSpec(memory_space=pltpu.VMEM),
        scratch_shapes=[
            pltpu.VMEM((width, hidden), bf16),
            pltpu.VMEM((2 * n, hidden, half), bf16),
            pltpu.VMEM((m - 1, own_rows, width), bf16),
            pltpu.VMEM((tokens, width), bf16),
            pltpu.VMEM((tokens, hidden), bf16),
            pltpu.VMEM((n, 2, tokens, half), bf16),
            pltpu.VMEM((m - 1, n, 2, own_rows, half), bf16),
            pltpu.VMEM((own_rows, width), jnp.float32),
            dma((2, n - 1, 2, 2)),
            dma((2, n - 1, 2, 2)),
            dma((m - 1,)),
            dma((m - 1,)),
            dma((m - 1,)),
            dma((m - 1,)),
            dma((m - 1, n)),
            dma((m - 1, n)),
        ],
        compiler_params=pltpu.CompilerParams(
            collective_id=0, has_side_effects=True, vmem_limit_bytes=60 * 1024 * 1024
        ),
    )(up_weight, down_weight, mix, residual, gains, biases)


def on_device(
    queries, keys, values, residual, sinks, out_weight, up_weight, down_weight, gains, biases
):
    tokens = queries.shape[0]
    rank_tp = lax.axis_index("tp")
    tails = jnp.stack([keys[tokens - WINDOW :], values[tokens - WINDOW :]])
    before = from_behind(tails, "sp", 1)
    offset = lax.axis_index("sp") * tokens
    attended = attend(queries, keys, values, before, sinks, offset, rank_tp)
    part = jnp.dot(attended, out_weight, preferred_element_type=jnp.float32).astype(jnp.bfloat16)
    if up_weight.shape[0] % (2 * LANES) == 0 and lax.axis_size("sp") % 2 == 0:
        return fused_block(up_weight, down_weight, part, residual, gains, biases)
    up_full, down_full = (
        lax.all_gather(up_weight, "sp", axis=0, tiled=True),
        lax.all_gather(down_weight, "sp", axis=1, tiled=True),
    )
    mix = lax.psum_scatter(
        part,
        "tp",
        scatter_dimension=0,
        tiled=True,
    ).astype(jnp.float32)
    normed = layer_norm(deep_alpha * residual.astype(jnp.float32) + mix, gains[0], biases[0])
    whole = lax.all_gather(normed, "tp", axis=0, tiled=True)
    upward = jnp.dot(whole, up_full, preferred_element_type=jnp.float32)
    act = jnp.square(jax.nn.relu(upward)).astype(jnp.bfloat16)
    terms = jnp.dot(act, down_full, preferred_element_type=jnp.float32)
    ffn = lax.psum_scatter(
        terms.astype(jnp.bfloat16), "tp", scatter_dimension=0, tiled=True
    ).astype(jnp.float32)
    return layer_norm(deep_alpha * normed.astype(jnp.float32) + ffn, gains[1], biases[1])


def solution(mesh):
    return jax.shard_map(
        on_device,
        mesh=mesh,
        in_specs=(
            P("sp", "tp"),
            P("sp", "tp"),
            P("sp", "tp"),
            P(("sp", "tp"), None),
            P("tp"),
            P("tp", None),
            P("sp", "tp"),
            P("tp", "sp"),
            P(),
            P(),
        ),
        out_specs=P(("sp", "tp"), None),
        check_vma=False,
    )
```

```python
import functools

import jax
import jax.numpy as jnp
from jax import lax
from jax.experimental import pallas as pl
from jax.experimental.pallas import tpu as pltpu
from jax.sharding import PartitionSpec as P

HEADS = 12
HEAD = 128
WINDOW = 128


deep_alpha = 1.6817928
norm_eps = 1e-05
neg_big = -1e30


def from_behind(block, axis, distance):
    devices = range(lax.axis_size(axis))
    route = [(i - distance, i) for i in devices if i - distance in devices]
    return lax.ppermute(block, axis, route)


def layer_norm(stream, gain, bias):
    mean = jnp.mean(stream, axis=-1, keepdims=True)
    spread = jnp.mean(jnp.square(stream - mean), axis=-1, keepdims=True)
    return ((stream - mean) * lax.rsqrt(spread + norm_eps) * gain + bias).astype(jnp.bfloat16)


def attend(queries, keys, values, before, sinks, offset, rank_tp):
    tokens = keys.shape[0]
    kv_local = keys.shape[1] // HEAD
    heads_local = sinks.shape[0]
    group = heads_local // kv_local
    blocks = tokens // WINDOW
    q_blocks = queries.reshape(blocks, WINDOW, kv_local, group, HEAD)
    key_ext = jnp.concatenate([before[0], keys], axis=0).reshape(tokens + WINDOW, kv_local, HEAD)
    val_ext = jnp.concatenate([before[1], values], axis=0).reshape(tokens + WINDOW, kv_local, HEAD)
    key_win = jnp.concatenate(
        [
            key_ext[:tokens].reshape(blocks, WINDOW, kv_local, HEAD),
            key_ext[WINDOW:].reshape(blocks, WINDOW, kv_local, HEAD),
        ],
        axis=1,
    )
    val_win = jnp.concatenate(
        [
            val_ext[:tokens].reshape(blocks, WINDOW, kv_local, HEAD),
            val_ext[WINDOW:].reshape(blocks, WINDOW, kv_local, HEAD),
        ],
        axis=1,
    )
    logits = jnp.einsum(
        "nqkgd,nskd->nkgqs", q_blocks, key_win, preferred_element_type=jnp.float32
    ) * HEAD ** (-0.5)
    q_index = jnp.arange(WINDOW, dtype=jnp.int32)[:, None]
    k_index = jnp.arange(2 * WINDOW, dtype=jnp.int32)[None, :]
    dist = q_index + WINDOW - k_index
    block_id = jnp.arange(blocks, dtype=jnp.int32)[:, None, None]
    key_pos = offset + block_id * WINDOW - WINDOW + k_index
    valid = (dist >= 0) & (dist < WINDOW) & (key_pos >= 0)
    heads = (jnp.arange(heads_local, dtype=jnp.int32) + rank_tp * heads_local).astype(jnp.float32)
    slopes = jnp.exp2(-8.0 * (heads + 1.0) / HEADS).reshape(kv_local, group)[:, :, None, None]
    logits = logits - slopes * dist.astype(jnp.float32)
    logits = jnp.where(valid[:, None, None], logits, neg_big)
    sink = sinks.reshape(kv_local, group)[:, :, None, None]
    top = jnp.maximum(jnp.max(logits, axis=-1, keepdims=True), sink)
    probs = jnp.exp(logits - top)
    denom = jnp.sum(probs, axis=-1, keepdims=True) + jnp.exp(sink - top)
    weight = (probs / denom).astype(jnp.bfloat16)
    attended = jnp.einsum("nkgqs,nskd->nqkgd", weight, val_win, preferred_element_type=jnp.float32)
    return attended.astype(jnp.bfloat16).reshape(tokens, heads_local * HEAD)


MESH = pl.DeviceIdType.MESH
LANES = 128


def norm_rows(stream, gain, bias):
    mean = jnp.mean(stream, axis=-1, keepdims=True)
    spread = jnp.mean(jnp.square(stream - mean), axis=-1, keepdims=True)
    return (stream - mean) * lax.rsqrt(spread + norm_eps) * gain + bias


def block_kernel(
    n, m, q_ref, k_ref, v_ref, sinks_ref, slopes_ref, proj_ref, up_ref, down_ref, res_ref,
    gains_ref, biases_ref, out_ref, key_ext, val_ext, attended, mix_ref, up_all, down_all, mix_in, normed, act, terms, terms_in, total,
    tail_send, tail_recv, ring_send, ring_recv, mix_send, mix_recv, row_send, row_recv, sum_send, sum_recv,
):
    me, rank = lax.axis_index("sp"), lax.axis_index("tp")
    depth, hidden = up_ref.shape
    half = depth // 2
    own_rows, width = res_ref.shape
    step_rows = 32

    odd = lax.rem(me, 2)
    place = (1 - odd) * lax.div(me, 2) + odd * (n - 1 - lax.div(me, 2))

    def member(at):
        at = lax.rem(at + n, n)
        back = lax.div(at, n // 2)
        return (1 - back) * (2 * at) + back * (2 * (n - 1 - at) + 1)

    right, left = member(place + 1), member(place - 1)

    def peer(k):
        return lax.rem(rank + k, m)

    barrier = pltpu.get_barrier_semaphore()
    after, ahead = lax.rem(me + 1, n), lax.rem(me + n - 1, n)
    for there in (left, right, after, ahead):
        pl.semaphore_signal(barrier, inc=1, device_id=(there, rank), device_id_type=MESH)
    for k in range(1, m):
        pl.semaphore_signal(barrier, inc=1, device_id=(me, peer(k)), device_id_type=MESH)
    pl.semaphore_wait(barrier, m + 3)

    def remote(source, target, send, recv, device):
        return pltpu.make_async_remote_copy(
            src_ref=source, dst_ref=target, send_sem=send, recv_sem=recv,
            device_id=device, device_id_type=MESH,
        )

    def hop(which, s, d, c):
        owner = member(place - s) if d == 0 else member(place + s)
        if which == 0:
            rows = half // 2
            off = d * half + c * rows
            target = up_all.at[pl.ds(pl.multiple_of(owner * depth + off, rows), rows)]
            source = up_ref.at[pl.ds(off, rows)] if s == 0 else target
        else:
            rows = hidden // 2
            target = down_all.at[2 * owner + d, pl.ds(c * rows, rows)]
            source = target
            if s == 0:
                source = down_ref.at[pl.ds(c * rows, rows), pl.ds(d * half, half)]
        return remote(
            source, target, ring_send.at[which, s, d, c], ring_recv.at[which, s, d, c],
            (right if d == 0 else left, rank),
        )

    def launch(which):
        for c in range(2):
            for d in range(2):
                hop(which, 0, d, c).start()

    def serve(which, s, c):
        for d in range(2):
            hop(which, s, d, c).wait_recv()
            if s + 1 < n - 1:
                hop(which, s + 1, d, c).start()

    def serve_up(s):
        for c in range(2):
            serve(0, s, c)
        if s == max(n - 3, 0):
            launch(1)

    tokens = q_ref.shape[0]
    tails = [
        remote(
            ref.at[pl.ds(tokens - WINDOW, WINDOW)], ext.at[pl.ds(0, WINDOW)],
            tail_send.at[i], tail_recv.at[i], (after, rank),
        )
        for i, (ref, ext) in enumerate(((k_ref, key_ext), (v_ref, val_ext)))
    ]
    for copy in tails:
        copy.start()
    launch(0)
    key_ext[WINDOW:] = k_ref[...]
    val_ext[WINDOW:] = v_ref[...]
    up_all[pl.ds(pl.multiple_of(me * depth, depth), depth)] = up_ref[...]
    for d in range(2):
        down_all[2 * me + d] = down_ref[:, d * half : (d + 1) * half]
    for copy in tails:
        copy.wait_recv()

    blocks = tokens // WINDOW
    heads_local = q_ref.shape[1] // HEAD
    group = heads_local // (k_ref.shape[1] // HEAD)

    def windows(first, last):
        @pl.loop(first, last)
        def _(i):
            start = pl.multiple_of(i * WINDOW, WINDOW)
            rows, span = pl.ds(start, WINDOW), pl.ds(start, 2 * WINDOW)
            q_index = lax.broadcasted_iota(jnp.int32, (WINDOW, 2 * WINDOW), 0)
            k_index = lax.broadcasted_iota(jnp.int32, (WINDOW, 2 * WINDOW), 1)
            dist = q_index + WINDOW - k_index
            key_pos = me * tokens + start - WINDOW + k_index
            valid = (dist >= 0) & (dist < WINDOW) & (key_pos >= 0)
            far = dist.astype(jnp.float32)
            for h in range(heads_local):
                columns = slice(h * HEAD, (h + 1) * HEAD)
                shared = slice(h // group * HEAD, (h // group + 1) * HEAD)
                logits = lax.dot_general(
                    q_ref[rows, columns], key_ext[span, shared], (((1,), (1,)), ((), ())),
                    preferred_element_type=jnp.float32,
                ) * HEAD ** (-0.5)
                logits = jnp.where(valid, logits - slopes_ref[h] * far, neg_big)
                sink = sinks_ref[h]
                top = jnp.maximum(jnp.max(logits, axis=-1, keepdims=True), sink)
                probs = jnp.exp(logits - top)
                denom = jnp.sum(probs, axis=-1, keepdims=True) + jnp.exp(sink - top)
                weight = (probs / denom).astype(jnp.bfloat16)
                attended[rows, columns] = jnp.dot(
                    weight, val_ext[span, shared], preferred_element_type=jnp.float32
                ).astype(jnp.bfloat16)

    windows(0, blocks // 2)
    serve(0, 0, 0)
    windows(blocks // 2, blocks)
    serve(0, 0, 1)

    @pl.loop(0, width // (2 * LANES))
    def _(i):
        columns = pl.ds(pl.multiple_of(i * 2 * LANES, 2 * LANES), 2 * LANES)
        mix_ref[:, columns] = jnp.dot(
            attended[...], proj_ref[:, columns], preferred_element_type=jnp.float32
        ).astype(jnp.bfloat16)

    mix_copies = [
        remote(
            mix_ref.at[pl.ds(pl.multiple_of(peer(k) * own_rows, own_rows), own_rows)],
            mix_in.at[k - 1], mix_send.at[k - 1], mix_recv.at[k - 1], (me, peer(k)),
        )
        for k in range(1, m)
    ]
    for copy in mix_copies:
        copy.start()

    early = n // 2
    for s in range(1, early):
        serve_up(s)
    for copy in mix_copies:
        copy.wait_recv()

    @pl.loop(0, own_rows // step_rows)
    def _(i):
        start = pl.multiple_of(i * step_rows, step_rows)
        rows = pl.ds(start, step_rows)
        mine = pl.ds(pl.multiple_of(rank * own_rows + start, step_rows), step_rows)
        mix = mix_ref[mine].astype(jnp.float32)
        for k in range(m - 1):
            mix += mix_in[k, rows].astype(jnp.float32)
        stream = deep_alpha * res_ref[rows].astype(jnp.float32) + mix
        normed[mine] = norm_rows(stream, gains_ref[0:1], biases_ref[0:1]).astype(jnp.bfloat16)

    held = pl.ds(pl.multiple_of(rank * own_rows, own_rows), own_rows)
    row_copies = [
        remote(
            normed.at[held], normed.at[held], row_send.at[k - 1], row_recv.at[k - 1], (me, peer(k))
        )
        for k in range(1, m)
    ]
    for copy in row_copies:
        copy.start()
    for s in range(early, n - 1):
        serve_up(s)
    for copy in row_copies:
        copy.wait_recv()

    tile = 256
    tiles = hidden // tile
    parts = 4

    def upward(first, last):
        @pl.loop(first, last)
        def _(i):
            columns = pl.ds(pl.multiple_of(i * tile, tile), tile)
            made = jnp.dot(normed[...], up_all[:, columns], preferred_element_type=jnp.float32)
            act[:, columns] = jnp.square(jnp.maximum(made, 0.0)).astype(jnp.bfloat16)

    for part in range(parts):
        upward(part * tiles // parts, (part + 1) * tiles // parts)
        if part < 2:
            serve(1, 0, part)

    def owners(j):
        return member(place - j), member(place + j)

    def share(j, k):
        return remote(
            terms.at[j, :, pl.ds(pl.multiple_of(peer(k) * own_rows, own_rows), own_rows)],
            terms_in.at[k - 1, j], sum_send.at[k - 1, j], sum_recv.at[k - 1, j], (me, peer(k)),
        )

    def downward(j):
        for d, owner in enumerate(owners(j)):
            terms[j, d] = jnp.dot(
                act[...], down_all[2 * owner + d], preferred_element_type=jnp.float32
            ).astype(jnp.bfloat16)
        for k in range(1, m):
            share(j, k).start()

    def collect(j):
        for k in range(1, m):
            share(j, k).wait_recv()
        for d, owner in enumerate(owners(j)):
            columns = pl.ds(pl.multiple_of(owner * depth + d * half, half), half)
            block = terms[j, d, held].astype(jnp.float32)
            for k in range(m - 1):
                block += terms_in[k, j, d].astype(jnp.float32)
            total[:, columns] = deep_alpha * normed[held, columns].astype(jnp.float32) + block

    downward(0)
    downward(1)
    for s in range(1, n - 1):
        for c in range(2):
            serve(1, s, c)
        downward(s + 1)
        collect(s - 1)
    collect(n - 2)
    collect(n - 1)

    @pl.loop(0, own_rows // step_rows)
    def _(i):
        rows = pl.ds(pl.multiple_of(i * step_rows, step_rows), step_rows)
        out_ref[rows] = norm_rows(total[rows], gains_ref[1:2], biases_ref[1:2]).astype(jnp.bfloat16)

    for copy in tails + mix_copies + row_copies:
        copy.wait_send()
    for j in range(n):
        for k in range(1, m):
            share(j, k).wait_send()
    for which in range(2):
        for s in range(n - 1):
            for d in range(2):
                for c in range(2):
                    hop(which, s, d, c).wait_send()


def fused_block(
    queries, keys, values, sinks, slopes, out_weight, up_weight, down_weight, residual, gains, biases
):
    n, m = lax.axis_size("sp"), lax.axis_size("tp")
    depth, hidden = up_weight.shape
    half = depth // 2
    tokens = queries.shape[0]
    own_rows, width = residual.shape
    vmem, smem = pl.BlockSpec(memory_space=pltpu.VMEM), pl.BlockSpec(memory_space=pltpu.SMEM)
    bf16, dma = jnp.bfloat16, pltpu.SemaphoreType.DMA
    return pl.pallas_call(
        functools.partial(block_kernel, n, m),
        out_shape=jax.ShapeDtypeStruct(residual.shape, bf16),
        in_specs=[vmem] * 3 + [smem] * 2 + [vmem] * 6,
        out_specs=pl.BlockSpec(memory_space=pltpu.VMEM),
        scratch_shapes=[
            pltpu.VMEM((tokens + WINDOW, keys.shape[1]), bf16),
            pltpu.VMEM((tokens + WINDOW, keys.shape[1]), bf16),
            pltpu.VMEM(queries.shape, bf16),
            pltpu.VMEM((tokens, width), bf16),
            pltpu.VMEM((width, hidden), bf16),
            pltpu.VMEM((2 * n, hidden, half), bf16),
            pltpu.VMEM((m - 1, own_rows, width), bf16),
            pltpu.VMEM((tokens, width), bf16),
            pltpu.VMEM((tokens, hidden), bf16),
            pltpu.VMEM((n, 2, tokens, half), bf16),
            pltpu.VMEM((m - 1, n, 2, own_rows, half), bf16),
            pltpu.VMEM((own_rows, width), jnp.float32),
            dma((2,)),
            dma((2,)),
            dma((2, n - 1, 2, 2)),
            dma((2, n - 1, 2, 2)),
            dma((m - 1,)),
            dma((m - 1,)),
            dma((m - 1,)),
            dma((m - 1,)),
            dma((m - 1, n)),
            dma((m - 1, n)),
        ],
        compiler_params=pltpu.CompilerParams(
            collective_id=0, has_side_effects=True, vmem_limit_bytes=60 * 1024 * 1024
        ),
    )(
        queries, keys, values, sinks, slopes, out_weight, up_weight, down_weight, residual, gains,
        biases,
    )


def on_device(
    queries, keys, values, residual, sinks, out_weight, up_weight, down_weight, gains, biases
):
    tokens = queries.shape[0]
    rank_tp = lax.axis_index("tp")
    if up_weight.shape[0] % (2 * LANES) == 0 and lax.axis_size("sp") % 2 == 0:
        heads_local = sinks.shape[0]
        heads = (jnp.arange(heads_local, dtype=jnp.int32) + rank_tp * heads_local).astype(jnp.float32)
        slopes = jnp.exp2(-8.0 * (heads + 1.0) / HEADS)
        return fused_block(
            queries, keys, values, sinks, slopes, out_weight, up_weight, down_weight, residual,
            gains, biases,
        )
    tails = jnp.stack([keys[tokens - WINDOW :], values[tokens - WINDOW :]])
    before = from_behind(tails, "sp", 1)
    offset = lax.axis_index("sp") * tokens
    attended = attend(queries, keys, values, before, sinks, offset, rank_tp)
    part = jnp.dot(attended, out_weight, preferred_element_type=jnp.float32).astype(jnp.bfloat16)
    up_full, down_full = (
        lax.all_gather(up_weight, "sp", axis=0, tiled=True),
        lax.all_gather(down_weight, "sp", axis=1, tiled=True),
    )
    mix = lax.psum_scatter(
        part,
        "tp",
        scatter_dimension=0,
        tiled=True,
    ).astype(jnp.float32)
    normed = layer_norm(deep_alpha * residual.astype(jnp.float32) + mix, gains[0], biases[0])
    whole = lax.all_gather(normed, "tp", axis=0, tiled=True)
    upward = jnp.dot(whole, up_full, preferred_element_type=jnp.float32)
    act = jnp.square(jax.nn.relu(upward)).astype(jnp.bfloat16)
    terms = jnp.dot(act, down_full, preferred_element_type=jnp.float32)
    ffn = lax.psum_scatter(
        terms.astype(jnp.bfloat16), "tp", scatter_dimension=0, tiled=True
    ).astype(jnp.float32)
    return layer_norm(deep_alpha * normed.astype(jnp.float32) + ffn, gains[1], biases[1])


def solution(mesh):
    return jax.shard_map(
        on_device,
        mesh=mesh,
        in_specs=(
            P("sp", "tp"),
            P("sp", "tp"),
            P("sp", "tp"),
            P(("sp", "tp"), None),
            P("tp"),
            P("tp", None),
            P("sp", "tp"),
            P("tp", "sp"),
            P(),
            P(),
        ),
        out_specs=P(("sp", "tp"), None),
        check_vma=False,
    )
```
